256 devices in a mesh: fs: 32 (over z, y), tp: 8 (over x, core).
Axes of the slice: x: 4, y: 4, z: 8, core: 2. Of those that a mesh axis runs over, the one named last changes fastest.
Arguments:
- cotangent: bfloat16 [32768, 4096], P(('fs', 'tp')), may hold values from -24 to 24
- gate_pre: bfloat16 [32768, 6144], P('fs', 'tp'), may hold values from -8 to 8
- up_pre: bfloat16 [32768, 6144], P('fs', 'tp'), may hold values from -6 to 6
- down_weight: bfloat16 [4096, 6144], P('fs', 'tp'), may hold values from -0.078125 to 0.078125
Outputs:
- gate_grad: bfloat16 [32768, 6144], P('fs', 'tp')
- up_grad: bfloat16 [32768, 6144], P('fs', 'tp')
- down_grad: float32 [4096, 6144], P('fs', 'tp')
The draws below stay inside these ranges and needn't reach their ends.
All inputs are finite; a program needn't handle non-finite values.
Results may differ from the reference program's by a relative error of at most 0.0027.
Values may be sent and summed in bfloat16 or wider, within the bound.
A program may use at most 128 MiB of HBM per device.

```python
import math
import jax
import jax.numpy as jnp
from jax import lax

D = 4096
FF = 6144
TOKENS = 32768


def raised(array, rng, source, target, parts, factor):
    def block_of(dim):
        return (jnp.arange(array.shape[dim]) // (array.shape[dim] // parts)).reshape((-1,) + (1,) * (array.ndim - 1 - dim))

    first = jax.random.permutation(rng, parts)[block_of(target)]
    second = (block_of(target) + parts // 2) % parts
    return jnp.where((block_of(source) == first) | (block_of(source) == second), factor * array, array)


def block_scale(rng, dims, pieces, least, largest):
    gain = 1.0
    for axis_at, blocks in pieces:
        steps = jax.random.uniform(jax.random.fold_in(jax.random.fold_in(rng, 6), axis_at), (blocks,), jnp.float32, least / len(pieces), largest / len(pieces))
        gain = gain * jnp.repeat(jnp.exp(steps), dims[axis_at] // blocks).reshape((-1,) + (1,) * (len(dims) - 1 - axis_at))
    return gain


def noise(rng, shape, scale, most, cuts=(), kind=jnp.bfloat16):
    entries = jax.random.normal(rng, shape, jnp.float32) * scale
    if len(cuts) > 0:
        entries = block_scale(rng, shape, cuts, -0.22, 0.18) * entries
    return jnp.clip(entries, min=-most, max=most).astype(kind)


def gaussian_with(stream_key, dims, scale, limit, cuts, heavy, held_as=jnp.bfloat16):
    drawn = scale * jax.random.normal(stream_key, dims, jnp.float32)
    if cuts:
        drawn = drawn * block_scale(stream_key, dims, cuts, -0.22, 0.18)
    return jnp.clip(raised(drawn, jax.random.fold_in(stream_key, 3), *heavy), -limit, limit).astype(held_as)


def setup_inputs(seed: int = 0) -> dict:
    splits = jax.random.split(jax.random.key(seed), 5)
    cotangent = gaussian_with(splits[0], (TOKENS, D), 1.0, 24.0, ((0, 256),), (0, 1, 256, 6.0))
    gate_pre = noise(splits[1], (TOKENS, FF), 1.5, 8.0, ((0, 32), (1, 8)))
    up_pre = noise(splits[2], (TOKENS, FF), 1.0, 6.0, ((0, 32), (1, 8)))
    down_weight = noise(splits[3], (D, FF), FF ** -0.5, 0.078125, ((0, 32), (1, 8)))
    return dict(cotangent=cotangent, gate_pre=gate_pre, up_pre=up_pre, down_weight=down_weight)


def reference(cotangent, gate_pre, up_pre, down_weight):
    gate_values = gate_pre.astype(jnp.float32)
    up_values = up_pre.astype(jnp.float32)
    sigmoid_gate = jax.nn.sigmoid(gate_values)
    silu_gate = gate_values * sigmoid_gate
    hidden = (silu_gate * up_values).astype(jnp.bfloat16)
    hidden_grad = 0.5 * jnp.dot(cotangent, down_weight, preferred_element_type=jnp.float32)
    up_grad = (hidden_grad * silu_gate).astype(jnp.bfloat16)
    gate_grad = (hidden_grad * up_values * sigmoid_gate * (1.0 + gate_values * (1.0 - sigmoid_gate))).astype(jnp.bfloat16)
    product = lax.dot_general(cotangent, hidden, (((0,), (0,)), ((), ())), preferred_element_type=jnp.float32)
    down_grad = product * (0.5 / math.sqrt(TOKENS))
    return (gate_grad, up_grad, down_grad)
```

```python
import math

import jax
import jax.numpy as jnp
from jax import lax
from jax.experimental import pallas as pl
from jax.experimental.pallas import tpu as pltpu
from jax.sharding import Mesh
from jax.sharding import PartitionSpec as P

ORDER = [
    0, 77, 78, 82, 1, 107, 97, 87, 39, 96, 59, 86, 106, 21, 43, 116, 35, 117, 73, 5, 88, 92, 27, 60, 65, 22,
    69, 31, 2, 45, 7, 40, 9, 47, 36, 74, 44, 6, 80, 84, 98, 83, 23, 61, 46, 28, 66, 8, 102, 32, 70, 49, 11,
    51, 13, 3, 41, 90, 94, 79, 48, 10, 24, 62, 85, 108, 112, 37, 75, 50, 12, 33, 67, 100, 52, 29, 71, 14, 15,
    53, 55, 81, 104, 17, 89, 93, 4, 42, 25, 63, 118, 188, 119, 185, 103, 143, 99, 138, 196, 193, 167, 139,
    189, 155, 162, 186, 110, 114, 179, 109, 113, 197, 163, 194, 68, 150, 57, 19, 76, 151, 72, 91, 95, 175, 64,
    140, 190, 187, 120, 105, 204, 201, 101, 145, 121, 205, 202, 164, 157, 169, 174, 156, 26, 152, 198, 144,
    122, 212, 195, 115, 123, 209, 219, 111, 181, 180, 38, 30, 34, 216, 168, 141, 220, 192, 124, 203, 206, 125,
    191, 217, 226, 158, 165, 210, 146, 227, 224, 214, 199, 211, 182, 221, 153, 218, 233, 170, 142, 223, 213,
    230, 208, 228, 200, 207, 231, 234, 176, 16, 147, 240, 166, 20, 58, 159, 154, 18, 235, 171, 225, 56, 215,
    232, 54, 222, 237, 177, 241, 148, 149, 183, 160, 242, 172, 238, 229, 128, 136, 236, 137, 178, 239, 133,
    132, 161, 173, 131, 129, 134, 126, 130, 127, 135, 243, 184,
]

NZ, NY, NX = 8, 4, 4
F32, BF16 = jnp.float32, jnp.bfloat16
BOTH = (1, -1)
ZORDER = [4, 3, -3, 2, -2, 1, -1, 0]
YORDER = [2, 1, -1, 0]
WA = 48
GA, GA_CUT, GB_CUT = 336, 176, 560
GROWS = {("A", 0): (0, GA_CUT), ("A", 1): (GA_CUT, GA), ("B", 0): (GA, GB_CUT), ("B", 1): (GB_CUT, 768)}
LINKS = [(a, s) for a in "zyx" for s in BOTH] + [("c", 1)]
BARRIER = len(LINKS)


def nz(v):
    return (v + 3) % 8 - 3


def ny(v):
    return (v + 1) % 4 - 1


def block_at(rz, ry):
    return ZORDER.index(nz(rz)) * 4 + YORDER.index(ny(ry))


def grows(part, half):
    if half is None:
        return GROWS[part, 0][0], GROWS[part, 1][1]
    return GROWS[part, half]


def step(rz, ry, axis, sign):
    return (nz(rz - sign), ry) if axis == "z" else (rz, ny(ry - sign))


class Tasks:
    def __init__(self, c):
        self.c = c
        self.tasks = []
        self.message = {}
        self.index = {}
        self.rows = {}
        self.total_rows = {BF16: 0, F32: 0}
        self.build()

    def task(self, name, needs, time, function=None, message=None):
        assert name not in self.index, name
        self.index[name] = len(self.tasks)
        if message:
            assert message[0] not in self.message
            self.message[message[0]] = len(self.message)
        self.tasks.append((name, tuple(needs), time, function, message))

    def weight(self, rz, ry, part, half, axis, sign, needs):
        tz, ty = step(rz, ry, axis, sign)
        r0, r1 = (0, WA) if part == "A" else (WA, 128)
        c0, c1 = (0, 768) if half is None else ((0, 384), (384, 768))[half]

        def at(z, y):
            b = block_at(z, y) * 128
            return lambda: self.c.w.at[pl.ds(b + r0, r1 - r0), pl.ds(c0, c1 - c0)]

        name = ("W", part, axis, sign, tz, ty)
        link, size = (axis, sign), (r1 - r0) * (c1 - c0) * 2
        self.task(("t",) + name, needs, 0.0, None, (name, link, size, at(rz, ry), at(tz, ty)))

    def cot(self, kind, piece, link, dx, half, needs):
        c = self.c
        h0, h1 = (0, 128) if half is None else ((0, 64), (64, 128))[half]

        def at():
            return c.cot.at[pl.ds(c.token_row(dx) + h0, h1 - h0), pl.ds(piece * 1024, 1024)]

        name = ("C", kind, piece, link)
        self.task(("t",) + name, needs, 0.0, None, (name, link, (h1 - h0) * 2048, at, at))

    def gradient(self, cls, part, half, axis, sign, rz, ry, needs, ins, kind):
        c = self.c
        tz, ty = step(rz, ry, axis, sign)
        name = (cls, half, sign, tz, ty)
        r0, r1 = grows(part, half)
        self.rows[name] = (kind, r0, r1, self.total_rows[kind])
        self.total_rows[kind] += r1 - r0
        self.task(
            ("t",) + name,
            list(needs) + list(ins),
            0.03,
            lambda: c.add(part, r0, r1, block_at(rz, ry), ins, name),
            (name, (axis, sign), (r1 - r0) * 128 * (2 if kind == BF16 else 4), lambda: c.slot("send", name), lambda: c.slot("recv", name)),
        )

    def build(self):
        c, weight, cot, task, gradient = self.c, self.weight, self.cot, self.task, self.gradient
        task("start", [], 2.5, lambda: c.start())
        start = ["start"]
        arrived = []
        for s in BOTH:
            h = 0 if s == 1 else 1
            weight(0, 0, "B", None, "z", s, start)
            for hop in (1, 2, 3):
                weight(-s * hop, 0, "B", h if hop == 3 else None, "z", s, [("W", "B", "z", s, -s * hop, 0)])
            for rz in [0, -1, 1, -2, 2, -3, 3, 4]:
                if rz == 0:
                    needs = start
                elif rz == 4:
                    needs = [("W", "B", "z", t, 4, 0) for t in BOTH]
                else:
                    needs = [("W", "B", "z", 1 if rz < 0 else -1, rz, 0)]
                weight(rz, 0, "B", None, "y", s, needs)
                weight(rz, -s, "B", h, "y", s, [("W", "B", "y", s, rz, -s)])
                arrived.append(("W", "B", "y", s, rz, 2))
            weight(0, 0, "A", None, "y", s, start)
            weight(0, -s, "A", h, "y", s, [("W", "A", "y", s, 0, -s)])
            for ry in YORDER:
                if ry == 0:
                    needs = start
                elif ry == 2:
                    needs = [("W", "A", "y", t, 0, 2) for t in BOTH]
                else:
                    needs = [("W", "A", "y", -ry, 0, ry)]
                weight(0, ry, "A", None, "z", s, needs)
                for hop in (1, 2, 3):
                    weight(-s * hop, ry, "A", h if hop == 3 else None, "z", s, [("W", "A", "z", s, -s * hop, ry)])
                arrived.append(("W", "A", "z", s, 4, ry))
        for k in range(4):
            task(("load", k), start, 0.0, lambda k=k: c.wait_cot_load(k))
            for s in BOTH:
                h = 0 if s == 1 else 1
                own = ("C", "own", k, ("x", s))
                cot("own", k, ("x", s), 0, None, [("load", k)])
                cot("forward", k, ("x", s), -s, h, [own])
                cot("side%d" % s, k, ("c", 1), -s, None, [own])
                cot("far%d" % s, k, ("c", 1), -2 * s, h, [("C", "forward", k, ("x", s))])
            cot("own", k, ("c", 1), 0, None, [("load", k)])
        task("hidden", start, 1.8, lambda: c.hidden())
        for i, rz in enumerate(ZORDER):
            k = i // 2
            pieces = [("C", kind, k, ("c", 1)) for kind in ("own", "side1", "side-1", "far1", "far-1")]
            pieces += [("C", kind, k, ("x", s)) for kind in ("own", "forward") for s in BOTH]
            task(("down", rz), ["hidden", ("load", k)] + pieces, 0.98, lambda i=i: c.down_product(i))
        for i in range(12):
            task(("hg", i), arrived + [("down", 0), ("down", 4), ("down", -3), ("down", -2)], 0.65, lambda i=i: c.hidden_grad(i))
        for ry in YORDER:
            for s in BOTH:
                h = 0 if s == 1 else 1
                gradient("A1", "A", h, "z", s, 4, ry, [("down", 4)], [], BF16)
                gradient("A1", "A", 1 - h, "z", s, 3 * s, ry, [("down", 3 * s)], [], BF16)
                gradient("A1", "A", h, "z", s, 3 * s, ry, [("down", 3 * s)], [("A1", h, s, 3 * s, ry)], BF16)
                gradient("A1", "A", None, "z", s, 2 * s, ry, [("down", 2 * s)], [("A1", v, s, 2 * s, ry) for v in (0, 1)], BF16)
                gradient("A1", "A", None, "z", s, s, ry, [("down", s)], [("A1", None, s, s, ry)], BF16)
            ins = [("A1", None, s, 0, ry) for s in BOTH]
            if ry == 2:
                for s in BOTH:
                    gradient("A2", "A", 0 if s == 1 else 1, "y", s, 0, 2, [("down", 0)], ins, F32)
            elif ry:
                h = 0 if ry == 1 else 1
                gradient("A2", "A", 1 - h, "y", ry, 0, ry, [("down", 0)], ins, F32)
                gradient("A2", "A", h, "y", ry, 0, ry, [("down", 0)], ins + [("A2", h, ry, 0, ry)], F32)
            else:
                ins = ins + [("A2", v, s, 0, 0) for s in BOTH for v in (0, 1)]
                task("finalA", ins + [("down", 0)], 0.05, lambda ins=ins: c.add("A", *grows("A", None), block_at(0, 0), ins, None))
        for rz in ZORDER:
            for s in BOTH:
                h = 0 if s == 1 else 1
                gradient("B1", "B", h, "y", s, rz, 2, [("down", rz)], [], BF16)
                gradient("B1", "B", 1 - h, "y", s, rz, s, [("down", rz)], [], BF16)
                gradient("B1", "B", h, "y", s, rz, s, [("down", rz)], [("B1", h, s, rz, s)], BF16)
            ins = [("B1", v, s, rz, 0) for s in BOTH for v in (0, 1)]
            if rz == 4:
                for s in BOTH:
                    gradient("B2", "B", 0 if s == 1 else 1, "z", s, 4, 0, [("down", 4)], ins, BF16)
            elif rz:
                s = 1 if rz > 0 else -1
                h = 0 if s == 1 else 1
                if abs(rz) == 3:
                    gradient("B2", "B", 1 - h, "z", s, rz, 0, [("down", rz)], ins, BF16)
                    gradient("B2", "B", h, "z", s, rz, 0, [("down", rz)], ins + [("B2", h, s, rz, 0)], BF16)
                elif abs(rz) == 2:
                    gradient("B2", "B", None, "z", s, rz, 0, [("down", rz)], ins + [("B2", v, s, rz, 0) for v in (0, 1)], BF16)
                else:
                    gradient("B2", "B", None, "z", s, rz, 0, [("down", rz)], ins + [("B2", None, s, rz, 0)], F32)
            else:
                ins = ins + [("B2", None, s, 0, 0) for s in BOTH]
                task("finalB", ins + [("down", 0)], 0.05, lambda ins=ins: c.add("B", *grows("B", None), block_at(0, 0), ins, None))


class Nothing:
    pass


class Kernel:
    def __init__(self, refs, scale):
        self.__dict__.update(refs)
        self.scale = scale
        self.z, self.y, self.x, self.core = (lax.axis_index(a) for a in ("z", "y", "x", "core"))
        self.pending = []

    def token_row(self, dx):
        return pl.multiple_of(lax.rem(self.x + dx + NX, NX) * 256 + self.core * 128, 128)

    def device(self, link):
        axis, sign = link
        if axis == "c":
            return {"core": 1 - self.core}
        size = {"z": NZ, "y": NY, "x": NX}[axis]
        return {axis: lax.rem(getattr(self, axis) + sign + size, size)}

    def local(self, src, dst, sem):
        copy = pltpu.make_async_copy(src, dst, self.lsem.at[sem])
        copy.start()
        return copy

    def start(self):
        barrier = pltpu.get_barrier_semaphore()
        for link in LINKS:
            pl.semaphore_signal(barrier, inc=1, device_id=self.device(link), device_id_type=pl.DeviceIdType.MESH)
        w_load = self.local(self.w_hbm, self.w.at[pl.ds(block_at(0, 0) * 128, 128)], 0)
        self.cot_loads = []
        own = self.token_row(0)
        for i, rz in enumerate(ZORDER):
            for j, ry in enumerate(YORDER):
                col = (lax.rem(self.z + rz + NZ, NZ) * NY + lax.rem(self.y + ry + NY, NY)) * 128
                b = i * 4 + j
                source = self.cot_hbm.at[:, pl.ds(pl.multiple_of(col, 128), 128)]
                self.cot_loads.append(self.local(source, self.cot.at[pl.ds(own, 128), pl.ds(b * 128, 128)], 3 + b))
        self.g_load = self.local(self.gate_hbm, self.gate, 1)
        self.u_load = self.local(self.up_hbm, self.up, 2)
        pl.semaphore_wait(barrier, BARRIER)
        w_load.wait()

    def wait_cot_load(self, k):
        for b in range(8 * k, 8 * k + 8):
            self.cot_loads[b].wait()

    def hidden(self):
        self.g_load.wait()
        self.u_load.wait()

        def body(i, carry):
            rows = pl.ds(pl.multiple_of(i * 128, 128), 128)
            for n in range(6):
                cols = pl.ds(n * 128, 128)
                g = self.gate[rows, cols].astype(F32)
                u = self.up[rows, cols].astype(F32)
                s = jax.nn.sigmoid(g)
                silu = g * s
                self.ht[cols, rows] = (silu * u).T.astype(BF16)
                self.to_up[rows, cols] = 0.5 * silu
                self.to_gate[rows, cols] = 0.5 * (u * s * (1.0 + g * (1.0 - s)))
            return carry

        lax.fori_loop(0, 8, body, 0)

    def down_product(self, z):
        for half in range(2):
            b = z * 4 + half * 2
            res = jnp.dot(self.ht[...], self.cot[:, pl.ds(b * 128, 256)], preferred_element_type=F32)
            self.part[b] = res[:, :128]
            self.part[b + 1] = res[:, 128:]

    def slot(self, side, name):
        kind, r0, r1, offset = self.rows[name]
        return self.buffers[side, kind].at[pl.ds(offset, r1 - r0)]

    def add(self, part, r0, r1, block, ins, name):
        spans = [self.rows[n] for n in ins]
        edges = {r0, r1} | {e for _, s0, s1, _ in spans for e in (s0, s1) if r0 < e < r1}
        cuts = sorted(edges)
        for a, b in zip(cuts, cuts[1:]):
            total = self.part[block, pl.ds(a, b - a)]
            for kind, s0, s1, offset in spans:
                if a >= s0 and b <= s1:
                    total = total + self.buffers["recv", kind][pl.ds(offset + a - s0, b - a)].astype(F32)
            if name is None:
                self.total[pl.ds(a, b - a)] = total
            else:
                kind, s0, _, offset = self.rows[name]
                self.buffers["send", kind][pl.ds(offset + a - s0, b - a)] = total.astype(kind)

    def hidden_grad(self, i):
        rows, cols = pl.ds(i // 3 * 256, 256), pl.ds(i % 3 * 256, 256)
        grad = jnp.dot(self.cot[rows], self.w[:, cols], preferred_element_type=F32)
        self.up_out[rows, cols] = (grad * self.to_up[rows, cols]).astype(BF16)
        self.gate_out[rows, cols] = (grad * self.to_gate[rows, cols]).astype(BF16)
        self.pending.append(self.local(self.gate_out.at[rows, cols], self.gate_grad.at[rows, cols], 35 + 2 * i))
        self.pending.append(self.local(self.up_out.at[rows, cols], self.up_grad.at[rows, cols], 36 + 2 * i))

    def finish(self):
        for n in range(6):
            rows = pl.ds(n * 128, 128)
            self.down_out[:, rows] = self.total[rows].T * self.scale
        self.pending.append(self.local(self.down_out, self.down_grad, 59))


def kernel(scale, cot_hbm, gate_hbm, up_hbm, w_hbm, gate_grad, up_grad, down_grad, cot, w, part, gate, up, to_gate, to_up, ht, gate_out, up_out, total, down_out, sb, rb, sf, rf, ssem, rsem, lsem):
    refs = dict(
        cot_hbm=cot_hbm, gate_hbm=gate_hbm, up_hbm=up_hbm, w_hbm=w_hbm,
        gate_grad=gate_grad, up_grad=up_grad, down_grad=down_grad,
        cot=cot, w=w, part=part, gate=gate, up=up, to_gate=to_gate, to_up=to_up, ht=ht,
        gate_out=gate_out, up_out=up_out, total=total, down_out=down_out, lsem=lsem,
        buffers={("send", BF16): sb, ("recv", BF16): rb, ("send", F32): sf, ("recv", F32): rf},
    )
    c = Kernel(refs, scale)
    p = Tasks(c)
    c.rows = p.rows
    copies, waited, done = {}, set(), set()
    assert sorted(ORDER) == list(range(len(p.tasks)))
    for t in ORDER:
        name, needs, _, function, message = p.tasks[t]
        for need in needs:
            if need in p.message:
                if need not in waited:
                    copies[need].wait_recv()
                    waited.add(need)
            else:
                assert need in done, need
        if function:
            function()
        if message:
            m, link, _, src, dst = message
            copies[m] = pltpu.make_async_remote_copy(
                src_ref=src(),
                dst_ref=dst(),
                send_sem=ssem.at[p.message[m]],
                recv_sem=rsem.at[p.message[m]],
                device_id=c.device(link),
                device_id_type=pl.DeviceIdType.MESH,
            )
            copies[m].start()
        done.add(name)
    assert waited == set(copies), set(copies) - waited
    c.finish()
    for m in copies:
        copies[m].wait_send()
    for copy in c.pending:
        copy.wait()


def local(cotangent, gate_pre, up_pre, down_weight):
    tokens = gate_pre.shape[0] * NZ * NY
    p = Tasks(Nothing())
    messages = len(p.message)
    hbm = pl.BlockSpec(memory_space=pl.ANY)

    def body(*refs):
        kernel(0.5 / math.sqrt(tokens), *refs)

    return pl.pallas_call(
        body,
        out_shape=(
            jax.ShapeDtypeStruct((1024, 768), BF16),
            jax.ShapeDtypeStruct((1024, 768), BF16),
            jax.ShapeDtypeStruct((128, 768), F32),
        ),
        in_specs=[hbm] * 4,
        out_specs=[hbm] * 3,
        scratch_shapes=[
            pltpu.VMEM((1024, 4096), BF16),
            pltpu.VMEM((4096, 768), BF16),
            pltpu.VMEM((32, 768, 128), F32),
            pltpu.VMEM((1024, 768), BF16),
            pltpu.VMEM((1024, 768), BF16),
            pltpu.VMEM((1024, 768), F32),
            pltpu.VMEM((1024, 768), F32),
            pltpu.VMEM((768, 1024), BF16),
            pltpu.VMEM((1024, 768), BF16),
            pltpu.VMEM((1024, 768), BF16),
            pltpu.VMEM((768, 128), F32),
            pltpu.VMEM((128, 768), F32),
            pltpu.VMEM((p.total_rows[BF16], 128), BF16),
            pltpu.VMEM((p.total_rows[BF16], 128), BF16),
            pltpu.VMEM((p.total_rows[F32], 128), F32),
            pltpu.VMEM((p.total_rows[F32], 128), F32),
            pltpu.SemaphoreType.DMA((messages,)),
            pltpu.SemaphoreType.DMA((messages,)),
            pltpu.SemaphoreType.DMA((60,)),
        ],
        compiler_params=pltpu.CompilerParams(
            collective_id=0, has_side_effects=True, vmem_limit_bytes=67043328
        ),
        name="gated_backward",
    )(cotangent, gate_pre, up_pre, down_weight)


def solution(mesh):
    torus = Mesh(mesh.devices.reshape(NZ, NY, NX, 2), ("z", "y", "x", "core"))
    rows, columns = ("z", "y"), ("x", "core")
    return jax.shard_map(
        local,
        mesh=torus,
        in_specs=(P(rows + columns, None), P(rows, columns), P(rows, columns), P(rows, columns)),
        out_specs=(P(rows, columns), P(rows, columns), P(rows, columns)),
        check_vma=False,
    )
```

```python
import math

import jax
import jax.numpy as jnp
from jax import lax
from jax.experimental import pallas as pl
from jax.experimental.pallas import tpu as pltpu
from jax.sharding import Mesh
from jax.sharding import PartitionSpec as P

ORDER = [
    0, 39, 77, 78, 82, 59, 1, 86, 87, 21, 107, 96, 97, 106, 35, 5, 43, 117, 73, 116, 88, 92, 65, 27, 60, 22,
    69, 31, 9, 40, 47, 2, 7, 45, 74, 36, 44, 6, 80, 84, 98, 102, 61, 23, 48, 10, 66, 28, 70, 32, 51, 13, 49,
    11, 41, 3, 90, 94, 79, 83, 46, 8, 62, 24, 89, 93, 67, 29, 52, 14, 71, 37, 100, 104, 108, 112, 50, 12, 75,
    33, 17, 55, 53, 15, 81, 85, 42, 4, 63, 25, 119, 185, 95, 91, 118, 180, 181, 154, 135, 131, 171, 103, 177,
    99, 188, 178, 159, 130, 120, 197, 121, 136, 193, 194, 160, 143, 142, 196, 172, 155, 54, 186, 109, 113,
    114, 110, 147, 167, 187, 148, 156, 182, 173, 166, 189, 179, 101, 105, 161, 132, 190, 19, 137, 38, 57, 64,
    144, 123, 111, 122, 195, 115, 149, 72, 34, 30, 68, 211, 26, 208, 76, 157, 212, 124, 223, 184, 125, 138,
    133, 198, 215, 225, 209, 174, 168, 204, 20, 183, 56, 201, 150, 191, 213, 210, 145, 162, 226, 202, 218,
    158, 217, 199, 227, 222, 200, 134, 206, 16, 139, 232, 192, 203, 205, 151, 169, 18, 58, 163, 229, 146, 220,
    216, 233, 214, 224, 219, 140, 234, 175, 230, 207, 141, 170, 128, 152, 164, 231, 127, 228, 221, 153, 129,
    165, 126, 235, 176,
]

NZ, NY, NX = 8, 4, 4
F32, BF16 = jnp.float32, jnp.bfloat16
BOTH = (1, -1)
ZORDER = [4, 3, -3, 2, -2, 1, -1, 0]
YORDER = [2, 1, -1, 0]
WA = 48
GA, GA_CUT, GB_CUT = 336, 176, 560
GROWS = {("A", 0): (0, GA_CUT), ("A", 1): (GA_CUT, GA), ("B", 0): (GA, GB_CUT), ("B", 1): (GB_CUT, 768)}
LINKS = [(a, s) for a in "zyx" for s in BOTH] + [("c", 1)]
BARRIER = len(LINKS)
OUTPUTS = [((1024, 768), BF16), ((1024, 768), BF16), ((128, 768), F32)]
LIMIT = 58 << 20


def nz(v):
    return (v + 3) % 8 - 3


def ny(v):
    return (v + 1) % 4 - 1


def block_at(rz, ry):
    return ZORDER.index(nz(rz)) * 4 + YORDER.index(ny(ry))


def grows(part, half):
    if half is None:
        return GROWS[part, 0][0], GROWS[part, 1][1]
    return GROWS[part, half]


def step(rz, ry, axis, sign):
    return (nz(rz - sign), ry) if axis == "z" else (rz, ny(ry - sign))


def send_group(message):
    return "WC".find(message[0]) if message[0] in "WC" else 2


def receive_group(message):
    if message[0] == "W":
        _, part, axis, _, rz, ry = message
        return ("W",) if (part, axis, ry) == ("B", "y", 2) or (part, axis, rz) == ("A", "z", 4) else message
    if message[0] == "C":
        return ("C", message[2]) if message[3][0] == "c" else message
    cls, _, s, rz, ry = message
    if cls in ("A2", "B1") and ry == 0 or cls != "B1" and rz == 0 and (cls, ry) != ("A2", 1) and (cls, ry) != ("A2", -1):
        return (cls, rz, ry)
    if abs(rz) == 2 and cls in ("A1", "B2"):
        return (cls, s, rz, ry)
    return message


def encode(value):
    value = value * 2.0**38
    return (value * jnp.abs(value)).astype(BF16)


def decode(coded):
    coded = coded.astype(F32)
    root = jnp.sqrt(jnp.abs(coded)) * 2.0**-38
    return jnp.where(coded < 0, -root, root)


class Tasks:
    def __init__(self, c):
        self.c = c
        self.tasks = []
        self.message = {}
        self.index = {}
        self.rows = {}
        self.total_rows = 0
        self.sent = [0, 0, 0]
        self.groups, self.group_size = {}, {}
        self.build()

    def task(self, name, needs, time, function=None, message=None):
        assert name not in self.index, name
        self.index[name] = len(self.tasks)
        if message:
            assert message[0] not in self.message
            self.message[message[0]] = len(self.message)
            self.sent[send_group(message[0])] += message[2] // 2
            key = receive_group(message[0])
            self.groups.setdefault(key, len(self.groups))
            self.group_size[key] = self.group_size.get(key, 0) + message[2] // 2
        self.tasks.append((name, tuple(needs), time, function, message))

    def weight(self, rz, ry, part, half, axis, sign, needs):
        tz, ty = step(rz, ry, axis, sign)
        r0, r1 = (0, WA) if part == "A" else (WA, 128)
        c0, c1 = (0, 768) if half is None else ((0, 384), (384, 768))[half]

        def at(z, y):
            b = block_at(z, y) * 128
            return lambda: self.c.w.at[pl.ds(b + r0, r1 - r0), pl.ds(c0, c1 - c0)]

        name = ("W", part, axis, sign, tz, ty)
        link, size = (axis, sign), (r1 - r0) * (c1 - c0) * 2
        self.task(("t",) + name, needs, 0.0, None, (name, link, size, at(rz, ry), at(tz, ty)))

    def cot(self, kind, piece, link, dx, half, needs):
        c = self.c
        h0, h1 = (0, 128) if half is None else ((0, 64), (64, 128))[half]

        def at():
            return c.cot.at[pl.ds(c.token_row(dx) + h0, h1 - h0), pl.ds(piece * 1024, 1024)]

        name = ("C", kind, piece, link)
        self.task(("t",) + name, needs, 0.0, None, (name, link, (h1 - h0) * 2048, at, at))

    def gradient(self, cls, part, half, axis, sign, rz, ry, needs, ins):
        c = self.c
        tz, ty = step(rz, ry, axis, sign)
        name = (cls, half, sign, tz, ty)
        r0, r1 = grows(part, half)
        self.rows[name] = (r0, r1, self.total_rows)
        self.total_rows += r1 - r0
        self.task(
            ("t",) + name,
            list(needs) + list(ins),
            0.03,
            lambda: c.add(part, r0, r1, block_at(rz, ry), ins, name),
            (name, (axis, sign), (r1 - r0) * 256, lambda: c.slot("send", name), lambda: c.slot("recv", name)),
        )

    def build(self):
        c, weight, cot, task, gradient = self.c, self.weight, self.cot, self.task, self.gradient
        task("start", [], 4.0, lambda: c.start())
        start = ["start"]
        arrived = []
        for s in BOTH:
            h = 0 if s == 1 else 1
            weight(0, 0, "B", None, "z", s, start)
            for hop in (1, 2, 3):
                weight(-s * hop, 0, "B", h if hop == 3 else None, "z", s, [("W", "B", "z", s, -s * hop, 0)])
            for rz in [0, -1, 1, -2, 2, -3, 3, 4]:
                if rz == 0:
                    needs = start
                elif rz == 4:
                    needs = [("W", "B", "z", t, 4, 0) for t in BOTH]
                else:
                    needs = [("W", "B", "z", 1 if rz < 0 else -1, rz, 0)]
                weight(rz, 0, "B", None, "y", s, needs)
                weight(rz, -s, "B", h, "y", s, [("W", "B", "y", s, rz, -s)])
                arrived.append(("W", "B", "y", s, rz, 2))
            weight(0, 0, "A", None, "y", s, start)
            weight(0, -s, "A", h, "y", s, [("W", "A", "y", s, 0, -s)])
            for ry in YORDER:
                if ry == 0:
                    needs = start
                elif ry == 2:
                    needs = [("W", "A", "y", t, 0, 2) for t in BOTH]
                else:
                    needs = [("W", "A", "y", -ry, 0, ry)]
                weight(0, ry, "A", None, "z", s, needs)
                for hop in (1, 2, 3):
                    weight(-s * hop, ry, "A", h if hop == 3 else None, "z", s, [("W", "A", "z", s, -s * hop, ry)])
                arrived.append(("W", "A", "z", s, 4, ry))
        for k in range(4):
            task(("load", k), start, 0.0, lambda k=k: c.wait_cot_load(k))
            for s in BOTH:
                h = 0 if s == 1 else 1
                own = ("C", "own", k, ("x", s))
                cot("own", k, ("x", s), 0, None, [("load", k)])
                cot("forward", k, ("x", s), -s, h, [own])
                cot("side%d" % s, k, ("c", 1), -s, None, [own])
                cot("far%d" % s, k, ("c", 1), -2 * s, h, [("C", "forward", k, ("x", s))])
            cot("own", k, ("c", 1), 0, None, [("load", k)])
        task("hidden", start, 2.0, lambda: c.hidden())
        for i, rz in enumerate(ZORDER):
            k = i // 2
            pieces = [("C", kind, k, ("c", 1)) for kind in ("own", "side1", "side-1", "far1", "far-1")]
            pieces += [("C", kind, k, ("x", s)) for kind in ("own", "forward") for s in BOTH]
            task(("down", rz), ["hidden", ("load", k)] + pieces, 1.0, lambda i=i: c.down_product(i))
        for i in range(4):
            task(("hg", i), arrived + [("down", rz) for rz in (4, -3, -2, 0)], 2.1, lambda i=i: c.hidden_grad(i))
        for ry in YORDER:
            for s in BOTH:
                h = 0 if s == 1 else 1
                gradient("A1", "A", h, "z", s, 4, ry, [("down", 4)], [])
                gradient("A1", "A", 1 - h, "z", s, 3 * s, ry, [("down", 3 * s)], [])
                gradient("A1", "A", h, "z", s, 3 * s, ry, [("down", 3 * s)], [("A1", h, s, 3 * s, ry)])
                gradient("A1", "A", None, "z", s, 2 * s, ry, [("down", 2 * s)], [("A1", v, s, 2 * s, ry) for v in (0, 1)])
                gradient("A1", "A", None, "z", s, s, ry, [("down", s)], [("A1", None, s, s, ry)])
            ins = [("A1", None, s, 0, ry) for s in BOTH]
            if ry == 2:
                for s in BOTH:
                    gradient("A2", "A", 0 if s == 1 else 1, "y", s, 0, 2, [("down", 0)], ins)
            elif ry:
                h = 0 if ry == 1 else 1
                gradient("A2", "A", 1 - h, "y", ry, 0, ry, [("down", 0)], ins)
                gradient("A2", "A", h, "y", ry, 0, ry, [("down", 0)], ins + [("A2", h, ry, 0, ry)])
            else:
                ins = ins + [("A2", v, s, 0, 0) for s in BOTH for v in (0, 1)]
                task("finalA", ins + [("down", 0)], 0.05, lambda ins=ins: c.add("A", *grows("A", None), block_at(0, 0), ins, None))
        for rz in ZORDER:
            for s in BOTH:
                h = 0 if s == 1 else 1
                gradient("B1", "B", h, "y", s, rz, 2, [("down", rz)], [])
                gradient("B1", "B", 1 - h, "y", s, rz, s, [("down", rz)], [])
                gradient("B1", "B", h, "y", s, rz, s, [("down", rz)], [("B1", h, s, rz, s)])
            ins = [("B1", v, s, rz, 0) for s in BOTH for v in (0, 1)]
            if rz == 4:
                for s in BOTH:
                    gradient("B2", "B", 0 if s == 1 else 1, "z", s, 4, 0, [("down", 4)], ins)
            elif rz:
                s = 1 if rz > 0 else -1
                h = 0 if s == 1 else 1
                if abs(rz) == 3:
                    gradient("B2", "B", 1 - h, "z", s, rz, 0, [("down", rz)], ins)
                    gradient("B2", "B", h, "z", s, rz, 0, [("down", rz)], ins + [("B2", h, s, rz, 0)])
                elif abs(rz) == 2:
                    gradient("B2", "B", None, "z", s, rz, 0, [("down", rz)], ins + [("B2", v, s, rz, 0) for v in (0, 1)])
                else:
                    gradient("B2", "B", None, "z", s, rz, 0, [("down", rz)], ins + [("B2", None, s, rz, 0)])
            else:
                ins = ins + [("B2", None, s, 0, 0) for s in BOTH]
                task("finalB", ins + [("down", 0)], 0.05, lambda ins=ins: c.add("B", *grows("B", None), block_at(0, 0), ins, None))


class Nothing:
    pass


class Kernel:
    def __init__(self, refs, scale):
        self.__dict__.update(refs)
        self.scale = scale
        self.z, self.y, self.x, self.core = (lax.axis_index(a) for a in ("z", "y", "x", "core"))

    def token_row(self, dx):
        return pl.multiple_of(lax.rem(self.x + dx + NX, NX) * 256 + self.core * 128, 128)

    def device(self, link):
        axis, sign = link
        if axis == "c":
            return {"core": 1 - self.core}
        size = {"z": NZ, "y": NY, "x": NX}[axis]
        return {axis: lax.rem(getattr(self, axis) + sign + size, size)}

    def local(self, src, dst, sem):
        copy = pltpu.make_async_copy(src, dst, self.lsem.at[sem])
        copy.start()
        return copy

    def start(self):
        barrier = pltpu.get_barrier_semaphore()
        for link in LINKS:
            pl.semaphore_signal(barrier, inc=1, device_id=self.device(link), device_id_type=pl.DeviceIdType.MESH)
        w_load = self.local(self.w_hbm, self.w.at[pl.ds(block_at(0, 0) * 128, 128)], 0)
        own = self.token_row(0)
        for i, rz in enumerate(ZORDER):
            for j, ry in enumerate(YORDER):
                col = (lax.rem(self.z + rz + NZ, NZ) * NY + lax.rem(self.y + ry + NY, NY)) * 128
                b = i * 4 + j
                source = self.cot_hbm.at[:, pl.ds(pl.multiple_of(col, 128), 128)]
                self.local(source, self.cot.at[pl.ds(own, 128), pl.ds(b * 128, 128)], 3 + b // 8)
        self.g_load = self.local(self.gate_hbm, self.gate, 1)
        self.u_load = self.local(self.up_hbm, self.up, 2)
        pl.semaphore_wait(barrier, BARRIER)
        w_load.wait()

    def wait_cot_load(self, k):
        piece = self.cot.at[pl.ds(0, 128), pl.ds(k * 1024, 1024)]
        pltpu.make_async_copy(piece, piece, self.lsem.at[3 + k]).wait()

    def hidden(self):
        self.g_load.wait()
        self.u_load.wait()

        def body(i, carry):
            rows = pl.ds(pl.multiple_of(i * 128, 128), 128)
            for n in range(6):
                cols = pl.ds(n * 128, 128)
                g = self.gate[rows, cols].astype(F32)
                u = self.up[rows, cols].astype(F32)
                s = jax.nn.sigmoid(g)
                silu = g * s
                self.ht[cols, rows] = (silu * u).T.astype(BF16)
                self.to_up[rows, cols] = 0.5 * silu
                self.to_gate[rows, cols] = 0.5 * (u * s * (1.0 + g * (1.0 - s)))
            return carry

        lax.fori_loop(0, 8, body, 0)

    def down_product(self, z):
        for half in range(2):
            b = z * 4 + half * 2
            res = jnp.dot(self.ht[...], self.cot[:, pl.ds(b * 128, 256)], preferred_element_type=F32)
            self.part[b] = res[:, :128]
            self.part[b + 1] = res[:, 128:]

    def slot(self, side, name):
        r0, r1, offset = self.rows[name]
        return self.buffers[side].at[pl.ds(offset, r1 - r0)]

    def add(self, part, r0, r1, block, ins, name):
        spans = [self.rows[n] for n in ins]
        edges = {r0, r1} | {e for s0, s1, _ in spans for e in (s0, s1) if r0 < e < r1}
        cuts = sorted(edges)
        for a, b in zip(cuts, cuts[1:]):
            total = self.part[block, pl.ds(a, b - a)]
            for s0, s1, offset in spans:
                if a >= s0 and b <= s1:
                    total = total + decode(self.buffers["recv"][pl.ds(offset + a - s0, b - a)])
            if name is None:
                self.total[pl.ds(a, b - a)] = total
            else:
                s0, _, offset = self.rows[name]
                self.buffers["send"][pl.ds(offset + a - s0, b - a)] = encode(total)

    def hidden_grad(self, i):
        def multiply(j, carry):
            rows = pl.ds(pl.multiple_of(i * 256 + j * 128, 128), 128)
            for n in range(3):
                cols = pl.ds(n * 256, 256)
                here = pl.ds(pl.multiple_of(j * 128, 128), 128)
                self.acc[here, cols] = jnp.dot(self.cot[rows], self.w[:, cols], preferred_element_type=F32)
            return carry

        def finish(j, carry):
            rows = pl.ds(pl.multiple_of(i * 256 + j * 32, 32), 32)
            grad = self.acc[pl.ds(pl.multiple_of(j * 32, 32), 32)]
            self.up_out[rows] = (grad * self.to_up[rows]).astype(BF16)
            self.gate_out[rows] = (grad * self.to_gate[rows]).astype(BF16)
            return carry

        lax.fori_loop(0, 2, multiply, 0)
        lax.fori_loop(0, 8, finish, 0, unroll=2)

    def finish(self):
        for n in range(6):
            rows = pl.ds(n * 128, 128)
            self.down_out[:, rows] = self.total[rows].T * self.scale


def kernel(scale, cot_hbm, gate_hbm, up_hbm, w_hbm, gate_out, up_out, down_out, cot, w, part, gate, up, to_gate, to_up, ht, acc, total, sb, rb, ssem, rsem, lsem):
    refs = dict(
        cot_hbm=cot_hbm, gate_hbm=gate_hbm, up_hbm=up_hbm, w_hbm=w_hbm,
        cot=cot, w=w, part=part, gate=gate, up=up, to_gate=to_gate, to_up=to_up, ht=ht,
        gate_out=gate_out, up_out=up_out, acc=acc, total=total, down_out=down_out, lsem=lsem,
        buffers={"send": sb, "recv": rb},
    )
    c = Kernel(refs, scale)
    p = Tasks(c)
    c.rows = p.rows
    waited, sent, done = set(), set(), set()
    assert sorted(ORDER) == list(range(len(p.tasks)))

    def all_of(kind, elements):
        ref = {"W": w, "C": cot}.get(kind, rb)
        assert elements % ref.shape[1] == 0
        return ref.at[pl.ds(0, elements // ref.shape[1])]

    def remote(src, dst, send, receive, link):
        return pltpu.make_async_remote_copy(
            src_ref=src,
            dst_ref=dst,
            send_sem=ssem.at[send],
            recv_sem=rsem.at[receive],
            device_id=c.device(link),
            device_id_type=pl.DeviceIdType.MESH,
        )

    for t in ORDER:
        name, needs, _, function, message = p.tasks[t]
        for need in needs:
            if need in p.message:
                key = receive_group(need)
                if key not in waited:
                    assert all(m in sent for m in p.message if receive_group(m) == key)
                    ref = all_of(need[0], p.group_size[key])
                    remote(ref, ref, 0, p.groups[key], LINKS[0]).wait_recv()
                    waited.add(key)
            else:
                assert need in done, need
        if function:
            function()
        if message:
            m, link, _, src, dst = message
            remote(src(), dst(), send_group(m), p.groups[receive_group(m)], link).start()
            sent.add(m)
        done.add(name)
    assert waited == set(p.groups), set(p.groups) - waited
    c.finish()
    for i, kind in enumerate("WCG"):
        ref = all_of(kind, p.sent[i])
        remote(ref, ref, i, 0, LINKS[0]).wait_send()


def copy_out(gate_in, up_in, down_in, gate_grad, up_grad, down_grad, sem):
    pairs = [(gate_in, gate_grad), (up_in, up_grad), (down_in, down_grad)]
    copies = [pltpu.make_async_copy(src, dst, sem.at[i]) for i, (src, dst) in enumerate(pairs)]
    for copy in copies:
        copy.start()
    for copy in copies:
        copy.wait()


def local(cotangent, gate_pre, up_pre, down_weight):
    tokens = gate_pre.shape[0] * NZ * NY
    p = Tasks(Nothing())
    hbm = pl.BlockSpec(memory_space=pl.ANY)

    def body(*refs):
        kernel(0.5 / math.sqrt(tokens), *refs)

    results = pl.pallas_call(
        body,
        out_shape=tuple(pltpu.VMEM(*o) for o in OUTPUTS),
        in_specs=[hbm] * 4,
        out_specs=[pl.BlockSpec(memory_space=pltpu.VMEM)] * 3,
        scratch_shapes=[
            pltpu.VMEM((1024, 4096), BF16),
            pltpu.VMEM((4096, 768), BF16),
            pltpu.VMEM((32, 768, 128), F32),
            pltpu.VMEM((1024, 768), BF16),
            pltpu.VMEM((1024, 768), BF16),
            pltpu.VMEM((1024, 768), F32),
            pltpu.VMEM((1024, 768), F32),
            pltpu.VMEM((768, 1024), BF16),
            pltpu.VMEM((256, 768), F32),
            pltpu.VMEM((768, 128), F32),
            pltpu.VMEM((p.total_rows, 128), BF16),
            pltpu.VMEM((p.total_rows, 128), BF16),
            pltpu.SemaphoreType.DMA((3,)),
            pltpu.SemaphoreType.DMA((len(p.groups),)),
            pltpu.SemaphoreType.DMA((7,)),
        ],
        compiler_params=pltpu.CompilerParams(
            collective_id=0, has_side_effects=True, vmem_limit_bytes=LIMIT
        ),
        name="gated_backward",
    )(cotangent, gate_pre, up_pre, down_weight)
    return pl.pallas_call(
        copy_out,
        out_shape=tuple(jax.ShapeDtypeStruct(*o) for o in OUTPUTS),
        in_specs=[pl.BlockSpec(memory_space=pltpu.VMEM)] * 3,
        out_specs=[hbm] * 3,
        scratch_shapes=[pltpu.SemaphoreType.DMA((3,))],
        compiler_params=pltpu.CompilerParams(vmem_limit_bytes=1 << 20),
        name="copy_out",
    )(*results)


def solution(mesh):
    torus = Mesh(mesh.devices.reshape(NZ, NY, NX, 2), ("z", "y", "x", "core"))
    rows, columns = ("z", "y"), ("x", "core")
    return jax.shard_map(
        local,
        mesh=torus,
        in_specs=(P(rows + columns, None), P(rows, columns), P(rows, columns), P(rows, columns)),
        out_specs=(P(rows, columns), P(rows, columns), P(rows, columns)),
        check_vma=False,
    )
```

```python
import math

import jax
import jax.numpy as jnp
from jax import lax
from jax.experimental import pallas as pl
from jax.experimental.pallas import tpu as pltpu
from jax.sharding import Mesh
from jax.sharding import PartitionSpec as P

ORDER = [
    0, 1, 97, 77, 82, 78, 107, 21, 39, 87, 96, 59, 5, 86, 106, 35, 117, 43, 116, 73, 112, 88, 31, 69, 22, 65,
    27, 60, 2, 7, 45, 40, 9, 47, 36, 74, 6, 44, 84, 80, 102, 79, 23, 61, 8, 28, 66, 46, 98, 32, 70, 49, 11,
    13, 51, 3, 41, 114, 90, 92, 10, 48, 24, 75, 81, 108, 29, 62, 12, 50, 37, 71, 104, 83, 14, 33, 67, 52, 15,
    53, 17, 100, 4, 113, 89, 55, 42, 25, 76, 63, 94, 93, 99, 30, 38, 72, 16, 34, 85, 110, 54, 68, 103, 109,
    19, 57, 118, 135, 154, 56, 177, 180, 91, 119, 185, 188, 130, 18, 147, 115, 159, 143, 155, 166, 171, 64,
    142, 186, 181, 95, 101, 167, 178, 189, 156, 20, 58, 120, 137, 149, 136, 179, 105, 132, 160, 196, 121, 194,
    161, 197, 131, 26, 111, 148, 123, 193, 182, 144, 172, 168, 122, 211, 187, 124, 190, 201, 173, 138, 157,
    125, 216, 133, 225, 162, 198, 126, 150, 183, 195, 208, 218, 204, 145, 128, 184, 213, 203, 191, 139, 215,
    205, 158, 209, 129, 199, 134, 222, 227, 163, 202, 212, 127, 192, 210, 200, 223, 206, 219, 146, 151, 220,
    217, 169, 226, 174, 229, 232, 224, 141, 230, 207, 164, 214, 140, 233, 152, 170, 231, 175, 234, 165, 221,
    228, 153, 176, 235,
]

NZ, NY, NX = 8, 4, 4
F32, BF16 = jnp.float32, jnp.bfloat16
BOTH = (1, -1)
ZORDER = [4, 3, -3, 2, -2, 1, -1, 0]
YORDER = [2, 1, -1, 0]
WA = 48
GA, GA_CUT, GB_CUT = 336, 176, 560
GROWS = {("A", 0): (0, GA_CUT), ("A", 1): (GA_CUT, GA), ("B", 0): (GA, GB_CUT), ("B", 1): (GB_CUT, 768)}
LINKS = [(a, s) for a in "zyx" for s in BOTH] + [("c", 1)]
BARRIER = len(LINKS)
OUTPUTS = [((1024, 768), BF16), ((1024, 768), BF16), ((128, 768), F32)]
LIMIT = 58 << 20


def nz(v):
    return (v + 3) % 8 - 3


def ny(v):
    return (v + 1) % 4 - 1


def block_at(rz, ry):
    return ZORDER.index(nz(rz)) * 4 + YORDER.index(ny(ry))


def grows(part, half):
    if half is None:
        return GROWS[part, 0][0], GROWS[part, 1][1]
    return GROWS[part, half]


def step(rz, ry, axis, sign):
    return (nz(rz - sign), ry) if axis == "z" else (rz, ny(ry - sign))


def send_group(message):
    return "WC".find(message[0]) if message[0] in "WC" else 2


def receive_group(message):
    if message[0] == "W":
        _, part, axis, _, rz, ry = message
        return ("W",) if (part, axis, ry) == ("B", "y", 2) or (part, axis, rz) == ("A", "z", 4) else message
    if message[0] == "C":
        return ("C", message[2]) if message[3][0] == "c" else message
    cls, _, s, rz, ry = message
    if cls in ("A2", "B1") and ry == 0 or cls != "B1" and rz == 0 and (cls, ry) != ("A2", 1) and (cls, ry) != ("A2", -1):
        return (cls, rz, ry)
    if abs(rz) == 2 and cls in ("A1", "B2"):
        return (cls, s, rz, ry)
    return message


def encode(value):
    value = value * 2.0**38
    return (value * jnp.abs(value)).astype(BF16)


def decode(coded):
    coded = coded.astype(F32)
    root = jnp.sqrt(jnp.abs(coded)) * 2.0**-38
    return jnp.where(coded < 0, -root, root)


class Tasks:
    def __init__(self, c):
        self.c = c
        self.tasks = []
        self.message = {}
        self.index = {}
        self.rows = {}
        self.total_rows = 0
        self.sent = [0, 0, 0]
        self.groups, self.group_size = {}, {}
        self.build()

    def task(self, name, needs, time, function=None, message=None):
        assert name not in self.index, name
        self.index[name] = len(self.tasks)
        if message:
            assert message[0] not in self.message
            self.message[message[0]] = len(self.message)
            self.sent[send_group(message[0])] += message[2] // 2
            key = receive_group(message[0])
            self.groups.setdefault(key, len(self.groups))
            self.group_size[key] = self.group_size.get(key, 0) + message[2] // 2
        self.tasks.append((name, tuple(needs), time, function, message))

    def weight(self, rz, ry, part, half, axis, sign, needs):
        tz, ty = step(rz, ry, axis, sign)
        r0, r1 = (0, WA) if part == "A" else (WA, 128)
        c0, c1 = (0, 768) if half is None else ((0, 384), (384, 768))[half]

        def at(z, y):
            b = block_at(z, y) * 128
            return lambda: self.c.w.at[pl.ds(b + r0, r1 - r0), pl.ds(c0, c1 - c0)]

        name = ("W", part, axis, sign, tz, ty)
        link, size = (axis, sign), (r1 - r0) * (c1 - c0) * 2
        self.task(("t",) + name, needs, 0.0, None, (name, link, size, at(rz, ry), at(tz, ty)))

    def cot(self, kind, piece, link, dx, half, needs):
        c = self.c
        h0, h1 = (0, 128) if half is None else ((0, 64), (64, 128))[half]

        def at():
            return c.cot.at[pl.ds(c.token_row(dx) + h0, h1 - h0), pl.ds(piece * 1024, 1024)]

        name = ("C", kind, piece, link)
        self.task(("t",) + name, needs, 0.0, None, (name, link, (h1 - h0) * 2048, at, at))

    def gradient(self, cls, part, half, axis, sign, rz, ry, needs, ins):
        c = self.c
        tz, ty = step(rz, ry, axis, sign)
        name = (cls, half, sign, tz, ty)
        r0, r1 = grows(part, half)
        self.rows[name] = (r0, r1, self.total_rows)
        self.total_rows += r1 - r0
        self.task(
            ("t",) + name,
            list(needs) + list(ins),
            0.05,
            lambda: c.add(part, r0, r1, block_at(rz, ry), ins, name),
            (name, (axis, sign), (r1 - r0) * 256, lambda: c.slot("send", name), lambda: c.slot("recv", name)),
        )

    def build(self):
        c, weight, cot, task, gradient = self.c, self.weight, self.cot, self.task, self.gradient
        task("start", [], 4.0, lambda: c.start())
        start = ["start"]
        arrived = []
        for s in BOTH:
            h = 0 if s == 1 else 1
            weight(0, 0, "B", None, "z", s, start)
            for hop in (1, 2, 3):
                weight(-s * hop, 0, "B", h if hop == 3 else None, "z", s, [("W", "B", "z", s, -s * hop, 0)])
            for rz in [0, -1, 1, -2, 2, -3, 3, 4]:
                if rz == 0:
                    needs = start
                elif rz == 4:
                    needs = [("W", "B", "z", t, 4, 0) for t in BOTH]
                else:
                    needs = [("W", "B", "z", 1 if rz < 0 else -1, rz, 0)]
                weight(rz, 0, "B", None, "y", s, needs)
                weight(rz, -s, "B", h, "y", s, [("W", "B", "y", s, rz, -s)])
                arrived.append(("W", "B", "y", s, rz, 2))
            weight(0, 0, "A", None, "y", s, start)
            weight(0, -s, "A", h, "y", s, [("W", "A", "y", s, 0, -s)])
            for ry in YORDER:
                if ry == 0:
                    needs = start
                elif ry == 2:
                    needs = [("W", "A", "y", t, 0, 2) for t in BOTH]
                else:
                    needs = [("W", "A", "y", -ry, 0, ry)]
                weight(0, ry, "A", None, "z", s, needs)
                for hop in (1, 2, 3):
                    weight(-s * hop, ry, "A", h if hop == 3 else None, "z", s, [("W", "A", "z", s, -s * hop, ry)])
                arrived.append(("W", "A", "z", s, 4, ry))
        for k in range(4):
            task(("load", k), start, 0.0, lambda k=k: c.wait_cot_load(k))
            for s in BOTH:
                h = 0 if s == 1 else 1
                own = ("C", "own", k, ("x", s))
                cot("own", k, ("x", s), 0, None, [("load", k)])
                cot("forward", k, ("x", s), -s, h, [own])
                cot("side%d" % s, k, ("c", 1), -s, None, [own])
                cot("far%d" % s, k, ("c", 1), -2 * s, h, [("C", "forward", k, ("x", s))])
            cot("own", k, ("c", 1), 0, None, [("load", k)])
        task("hidden", start, 2.0, lambda: c.hidden())
        for i, rz in enumerate(ZORDER):
            k = i // 2
            pieces = [("C", kind, k, ("c", 1)) for kind in ("own", "side1", "side-1", "far1", "far-1")]
            pieces += [("C", kind, k, ("x", s)) for kind in ("own", "forward") for s in BOTH]
            task(("down", rz), ["hidden", ("load", k)] + pieces, 1.0, lambda i=i: c.down_product(i))
        for i in range(4):
            task(("hg", i), arrived + [("down", rz) for rz in (4, -3, -2, 0)], 2.1, lambda i=i: c.hidden_grad(i))
        for ry in YORDER:
            for s in BOTH:
                h = 0 if s == 1 else 1
                gradient("A1", "A", h, "z", s, 4, ry, [("down", 4)], [])
                gradient("A1", "A", 1 - h, "z", s, 3 * s, ry, [("down", 3 * s)], [])
                gradient("A1", "A", h, "z", s, 3 * s, ry, [("down", 3 * s)], [("A1", h, s, 3 * s, ry)])
                gradient("A1", "A", None, "z", s, 2 * s, ry, [("down", 2 * s)], [("A1", v, s, 2 * s, ry) for v in (0, 1)])
                gradient("A1", "A", None, "z", s, s, ry, [("down", s)], [("A1", None, s, s, ry)])
            ins = [("A1", None, s, 0, ry) for s in BOTH]
            if ry == 2:
                for s in BOTH:
                    gradient("A2", "A", 0 if s == 1 else 1, "y", s, 0, 2, [("down", 0)], ins)
            elif ry:
                h = 0 if ry == 1 else 1
                gradient("A2", "A", 1 - h, "y", ry, 0, ry, [("down", 0)], ins)
                gradient("A2", "A", h, "y", ry, 0, ry, [("down", 0)], ins + [("A2", h, ry, 0, ry)])
            else:
                ins = ins + [("A2", v, s, 0, 0) for s in BOTH for v in (0, 1)]
                task("finalA", ins + [("down", 0)], 0.05, lambda ins=ins: c.add("A", *grows("A", None), block_at(0, 0), ins, None))
        for rz in ZORDER:
            for s in BOTH:
                h = 0 if s == 1 else 1
                gradient("B1", "B", h, "y", s, rz, 2, [("down", rz)], [])
                gradient("B1", "B", 1 - h, "y", s, rz, s, [("down", rz)], [])
                gradient("B1", "B", h, "y", s, rz, s, [("down", rz)], [("B1", h, s, rz, s)])
            ins = [("B1", v, s, rz, 0) for s in BOTH for v in (0, 1)]
            if rz == 4:
                for s in BOTH:
                    gradient("B2", "B", 0 if s == 1 else 1, "z", s, 4, 0, [("down", 4)], ins)
            elif rz:
                s = 1 if rz > 0 else -1
                h = 0 if s == 1 else 1
                if abs(rz) == 3:
                    gradient("B2", "B", 1 - h, "z", s, rz, 0, [("down", rz)], ins)
                    gradient("B2", "B", h, "z", s, rz, 0, [("down", rz)], ins + [("B2", h, s, rz, 0)])
                elif abs(rz) == 2:
                    gradient("B2", "B", None, "z", s, rz, 0, [("down", rz)], ins + [("B2", v, s, rz, 0) for v in (0, 1)])
                else:
                    gradient("B2", "B", None, "z", s, rz, 0, [("down", rz)], ins + [("B2", None, s, rz, 0)])
            else:
                ins = ins + [("B2", None, s, 0, 0) for s in BOTH]
                task("finalB", ins + [("down", 0)], 0.05, lambda ins=ins: c.add("B", *grows("B", None), block_at(0, 0), ins, None))


class Nothing:
    pass


class Kernel:
    def __init__(self, refs, scale):
        self.__dict__.update(refs)
        self.scale = scale
        self.z, self.y, self.x, self.core = (lax.axis_index(a) for a in ("z", "y", "x", "core"))

    def token_row(self, dx):
        return pl.multiple_of(lax.rem(self.x + dx + NX, NX) * 256 + self.core * 128, 128)

    def device(self, link):
        axis, sign = link
        if axis == "c":
            return {"core": 1 - self.core}
        size = {"z": NZ, "y": NY, "x": NX}[axis]
        return {axis: lax.rem(getattr(self, axis) + sign + size, size)}

    def local(self, src, dst, sem):
        copy = pltpu.make_async_copy(src, dst, self.lsem.at[sem])
        copy.start()
        return copy

    def start(self):
        barrier = pltpu.get_barrier_semaphore()
        for link in LINKS:
            pl.semaphore_signal(barrier, inc=1, device_id=self.device(link), device_id_type=pl.DeviceIdType.MESH)
        w_load = self.local(self.w_hbm, self.w.at[pl.ds(block_at(0, 0) * 128, 128)], 0)
        own = self.token_row(0)
        for i, rz in enumerate(ZORDER):
            for j, ry in enumerate(YORDER):
                col = (lax.rem(self.z + rz + NZ, NZ) * NY + lax.rem(self.y + ry + NY, NY)) * 128
                b = i * 4 + j
                source = self.cot_hbm.at[:, pl.ds(pl.multiple_of(col, 128), 128)]
                self.local(source, self.cot.at[pl.ds(own, 128), pl.ds(b * 128, 128)], 3 + b // 8)
        self.g_load = self.local(self.gate_hbm, self.gate, 1)
        self.u_load = self.local(self.up_hbm, self.up, 2)
        pl.semaphore_wait(barrier, BARRIER)
        w_load.wait()

    def wait_cot_load(self, k):
        piece = self.cot.at[pl.ds(0, 128), pl.ds(k * 1024, 1024)]
        pltpu.make_async_copy(piece, piece, self.lsem.at[3 + k]).wait()

    def hidden(self):
        self.g_load.wait()
        self.u_load.wait()

        def body(i, carry):
            rows = pl.ds(pl.multiple_of(i * 128, 128), 128)
            for n in range(6):
                cols = pl.ds(n * 128, 128)
                g = self.gate[rows, cols].astype(F32)
                u = self.up[rows, cols].astype(F32)
                s = jax.nn.sigmoid(g)
                silu = g * s
                self.ht[cols, rows] = (silu * u).T.astype(BF16)
                self.to_up[rows, cols] = 0.5 * silu
                self.to_gate[rows, cols] = 0.5 * (u * s * (1.0 + g * (1.0 - s)))
            return carry

        lax.fori_loop(0, 8, body, 0)

    def down_product(self, z):
        for half in range(2):
            b = z * 4 + half * 2
            res = jnp.dot(self.ht[...], self.cot[:, pl.ds(b * 128, 256)], preferred_element_type=F32)
            self.part[b] = res[:, :128]
            self.part[b + 1] = res[:, 128:]

    def slot(self, side, name):
        r0, r1, offset = self.rows[name]
        return self.buffers[side].at[pl.ds(offset, r1 - r0)]

    def add(self, part, r0, r1, block, ins, name):
        spans = [self.rows[n] for n in ins]
        edges = {r0, r1} | {e for s0, s1, _ in spans for e in (s0, s1) if r0 < e < r1}
        cuts = sorted(edges)
        for a, b in zip(cuts, cuts[1:]):
            total = self.part[block, pl.ds(a, b - a)]
            for s0, s1, offset in spans:
                if a >= s0 and b <= s1:
                    total = total + decode(self.buffers["recv"][pl.ds(offset + a - s0, b - a)])
            if name is None:
                self.total[pl.ds(a, b - a)] = total
            else:
                s0, _, offset = self.rows[name]
                self.buffers["send"][pl.ds(offset + a - s0, b - a)] = encode(total)

    def hidden_grad(self, i):
        def multiply(j, carry):
            rows = pl.ds(pl.multiple_of(i * 256 + j * 128, 128), 128)
            for n in range(3):
                cols = pl.ds(n * 256, 256)
                here = pl.ds(pl.multiple_of(j * 128, 128), 128)
                self.acc[here, cols] = jnp.dot(self.cot[rows], self.w[:, cols], preferred_element_type=F32)
            return carry

        def finish(j, carry):
            rows = pl.ds(pl.multiple_of(i * 256 + j * 32, 32), 32)
            grad = self.acc[pl.ds(pl.multiple_of(j * 32, 32), 32)]
            self.up_out[rows] = (grad * self.to_up[rows]).astype(BF16)
            self.gate_out[rows] = (grad * self.to_gate[rows]).astype(BF16)
            return carry

        lax.fori_loop(0, 2, multiply, 0)
        lax.fori_loop(0, 8, finish, 0, unroll=2)

    def finish(self):
        for n in range(6):
            rows = pl.ds(n * 128, 128)
            self.down_out[:, rows] = self.total[rows].T * self.scale


def kernel(scale, cot_hbm, gate_hbm, up_hbm, w_hbm, gate_out, up_out, down_out, cot, w, part, gate, up, to_gate, to_up, ht, acc, total, sb, rb, ssem, rsem, lsem):
    refs = dict(
        cot_hbm=cot_hbm, gate_hbm=gate_hbm, up_hbm=up_hbm, w_hbm=w_hbm,
        cot=cot, w=w, part=part, gate=gate, up=up, to_gate=to_gate, to_up=to_up, ht=ht,
        gate_out=gate_out, up_out=up_out, acc=acc, total=total, down_out=down_out, lsem=lsem,
        buffers={"send": sb, "recv": rb},
    )
    c = Kernel(refs, scale)
    p = Tasks(c)
    c.rows = p.rows
    waited, sent, done = set(), set(), set()
    assert sorted(ORDER) == list(range(len(p.tasks)))

    def all_of(kind, elements):
        ref = {"W": w, "C": cot}.get(kind, rb)
        assert elements % ref.shape[1] == 0
        return ref.at[pl.ds(0, elements // ref.shape[1])]

    def remote(src, dst, send, receive, link):
        return pltpu.make_async_remote_copy(
            src_ref=src,
            dst_ref=dst,
            send_sem=ssem.at[send],
            recv_sem=rsem.at[receive],
            device_id=c.device(link),
            device_id_type=pl.DeviceIdType.MESH,
        )

    for t in ORDER:
        name, needs, _, function, message = p.tasks[t]
        for need in needs:
            if need in p.message:
                key = receive_group(need)
                if key not in waited:
                    assert all(m in sent for m in p.message if receive_group(m) == key)
                    ref = all_of(need[0], p.group_size[key])
                    remote(ref, ref, 0, p.groups[key], LINKS[0]).wait_recv()
                    waited.add(key)
            else:
                assert need in done, need
        if function:
            function()
        if message:
            m, link, _, src, dst = message
            remote(src(), dst(), send_group(m), p.groups[receive_group(m)], link).start()
            sent.add(m)
        done.add(name)
    assert waited == set(p.groups), set(p.groups) - waited
    c.finish()
    for i, kind in enumerate("WCG"):
        ref = all_of(kind, p.sent[i])
        remote(ref, ref, i, 0, LINKS[0]).wait_send()


def copy_out(gate_in, up_in, down_in, gate_grad, up_grad, down_grad, sem):
    pairs = [(gate_in, gate_grad), (up_in, up_grad), (down_in, down_grad)]
    copies = [pltpu.make_async_copy(src, dst, sem.at[i]) for i, (src, dst) in enumerate(pairs)]
    for copy in copies:
        copy.start()
    for copy in copies:
        copy.wait()


def local(cotangent, gate_pre, up_pre, down_weight):
    tokens = gate_pre.shape[0] * NZ * NY
    p = Tasks(Nothing())
    hbm = pl.BlockSpec(memory_space=pl.ANY)

    def body(*refs):
        kernel(0.5 / math.sqrt(tokens), *refs)

    results = pl.pallas_call(
        body,
        out_shape=tuple(pltpu.VMEM(*o) for o in OUTPUTS),
        in_specs=[hbm] * 4,
        out_specs=[pl.BlockSpec(memory_space=pltpu.VMEM)] * 3,
        scratch_shapes=[
            pltpu.VMEM((1024, 4096), BF16),
            pltpu.VMEM((4096, 768), BF16),
            pltpu.VMEM((32, 768, 128), F32),
            pltpu.VMEM((1024, 768), BF16),
            pltpu.VMEM((1024, 768), BF16),
            pltpu.VMEM((1024, 768), F32),
            pltpu.VMEM((1024, 768), F32),
            pltpu.VMEM((768, 1024), BF16),
            pltpu.VMEM((256, 768), F32),
            pltpu.VMEM((768, 128), F32),
            pltpu.VMEM((p.total_rows, 128), BF16),
            pltpu.VMEM((p.total_rows, 128), BF16),
            pltpu.SemaphoreType.DMA((3,)),
            pltpu.SemaphoreType.DMA((len(p.groups),)),
            pltpu.SemaphoreType.DMA((7,)),
        ],
        compiler_params=pltpu.CompilerParams(
            collective_id=0, has_side_effects=True, vmem_limit_bytes=LIMIT
        ),
        name="gated_backward",
    )(cotangent, gate_pre, up_pre, down_weight)
    return pl.pallas_call(
        copy_out,
        out_shape=tuple(jax.ShapeDtypeStruct(*o) for o in OUTPUTS),
        in_specs=[pl.BlockSpec(memory_space=pltpu.VMEM)] * 3,
        out_specs=[hbm] * 3,
        scratch_shapes=[pltpu.SemaphoreType.DMA((3,))],
        compiler_params=pltpu.CompilerParams(vmem_limit_bytes=1 << 20),
        name="copy_out",
    )(*results)


def solution(mesh):
    torus = Mesh(mesh.devices.reshape(NZ, NY, NX, 2), ("z", "y", "x", "core"))
    rows, columns = ("z", "y"), ("x", "core")
    return jax.shard_map(
        local,
        mesh=torus,
        in_specs=(P(rows + columns, None), P(rows, columns), P(rows, columns), P(rows, columns)),
        out_specs=(P(rows, columns), P(rows, columns), P(rows, columns)),
        check_vma=False,
    )
```

```python
import math

import jax
import jax.numpy as jnp
from jax import lax
from jax.experimental import pallas as pl
from jax.experimental.pallas import tpu as pltpu
from jax.sharding import Mesh
from jax.sharding import PartitionSpec as P

ORDER = [
    0, 1, 97, 77, 82, 78, 107, 21, 39, 87, 96, 59, 5, 86, 106, 35, 117, 43, 116, 73, 112, 88, 31, 69, 22, 65,
    27, 60, 2, 7, 45, 40, 9, 47, 36, 74, 6, 44, 84, 80, 102, 79, 23, 61, 8, 28, 66, 46, 98, 32, 70, 49, 11,
    13, 51, 3, 41, 114, 90, 92, 10, 48, 24, 75, 81, 108, 29, 62, 12, 50, 37, 71, 104, 83, 14, 33, 67, 52, 15,
    53, 17, 100, 4, 113, 89, 55, 42, 25, 76, 63, 94, 93, 99, 30, 38, 72, 16, 34, 85, 110, 54, 68, 103, 109,
    19, 57, 118, 135, 154, 56, 177, 180, 91, 119, 185, 188, 130, 18, 147, 115, 159, 143, 155, 166, 171, 64,
    142, 186, 181, 95, 101, 167, 178, 189, 156, 20, 58, 120, 137, 149, 136, 179, 105, 132, 160, 196, 121, 194,
    161, 197, 131, 26, 111, 148, 123, 193, 182, 144, 172, 168, 122, 211, 187, 124, 190, 201, 173, 138, 157,
    125, 216, 133, 225, 162, 198, 126, 150, 183, 195, 208, 218, 204, 145, 128, 184, 213, 203, 191, 139, 215,
    205, 158, 209, 129, 199, 134, 222, 227, 163, 202, 212, 127, 192, 210, 200, 223, 206, 219, 146, 151, 220,
    217, 169, 226, 174, 229, 232, 224, 141, 230, 207, 164, 214, 140, 233, 152, 170, 231, 175, 234, 165, 221,
    228, 153, 176, 235,
]

NZ, NY, NX = 8, 4, 4
F32, BF16 = jnp.float32, jnp.bfloat16
BOTH = (1, -1)
ZORDER = [4, 3, -3, 2, -2, 1, -1, 0]
YORDER = [2, 1, -1, 0]
WA = 48
GA, GA_CUT, GB_CUT = 336, 176, 560
GROWS = {("A", 0): (0, GA_CUT), ("A", 1): (GA_CUT, GA), ("B", 0): (GA, GB_CUT), ("B", 1): (GB_CUT, 768)}
LINKS = [(a, s) for a in "zyx" for s in BOTH] + [("c", 1)]
BARRIER = len(LINKS)
OUTPUTS = [((1024, 768), BF16), ((1024, 768), BF16), ((128, 768), F32)]
LIMIT = 58 << 20


def nz(v):
    return (v + 3) % 8 - 3


def ny(v):
    return (v + 1) % 4 - 1


def block_at(rz, ry):
    return ZORDER.index(nz(rz)) * 4 + YORDER.index(ny(ry))


def grows(part, half):
    if half is None:
        return GROWS[part, 0][0], GROWS[part, 1][1]
    return GROWS[part, half]


def step(rz, ry, axis, sign):
    return (nz(rz - sign), ry) if axis == "z" else (rz, ny(ry - sign))


def send_group(message):
    return "WC".find(message[0]) if message[0] in "WC" else 2


def receive_group(message):
    if message[0] == "W":
        _, part, axis, _, rz, ry = message
        last = (part, axis, ry) == ("B", "y", 2) or (part, axis, rz) == ("A", "z", 4)
        return ("W",) if last else ("W", part, axis, abs(rz) if axis == "z" else rz, abs(ry) if axis == "y" else ry)
    if message[0] == "C":
        return ("C", message[2]) if message[3][0] == "c" else message
    cls, _, s, rz, ry = message
    if cls in ("A2", "B1") and ry == 0 or cls != "B1" and rz == 0 and (cls, ry) != ("A2", 1) and (cls, ry) != ("A2", -1):
        return (cls, rz, ry)
    if abs(rz) == 2 and cls in ("A1", "B2"):
        return (cls, s, rz, ry)
    return message


def encode(value):
    value = value * 2.0**38
    return (value * jnp.abs(value)).astype(BF16)


def decode(coded):
    coded = coded.astype(F32)
    root = jnp.sqrt(jnp.abs(coded)) * 2.0**-38
    return jnp.where(coded < 0, -root, root)


class Tasks:
    def __init__(self, c):
        self.c = c
        self.tasks = []
        self.message = {}
        self.index = {}
        self.rows = {}
        self.total_rows = 0
        self.sent = [0, 0, 0]
        self.groups, self.group_size = {}, {}
        self.build()
        for i, (name, needs, *rest) in enumerate(self.tasks):
            keys = {receive_group(n) for n in needs if n in self.message}
            whole = [m for m in self.message if receive_group(m) in keys]
            self.tasks[i] = (name, tuple(n for n in needs if n not in self.message) + tuple(whole), *rest)

    def task(self, name, needs, time, function=None, message=None):
        assert name not in self.index, name
        self.index[name] = len(self.tasks)
        if message:
            assert message[0] not in self.message
            self.message[message[0]] = len(self.message)
            self.sent[send_group(message[0])] += message[2] // 2
            key = receive_group(message[0])
            self.groups.setdefault(key, len(self.groups))
            self.group_size[key] = self.group_size.get(key, 0) + message[2] // 2
        self.tasks.append((name, tuple(needs), time, function, message))

    def weight(self, rz, ry, part, half, axis, sign, needs):
        tz, ty = step(rz, ry, axis, sign)
        r0, r1 = (0, WA) if part == "A" else (WA, 128)
        c0, c1 = (0, 768) if half is None else ((0, 384), (384, 768))[half]

        def at(z, y):
            b = block_at(z, y) * 128
            return lambda: self.c.w.at[pl.ds(b + r0, r1 - r0), pl.ds(c0, c1 - c0)]

        name = ("W", part, axis, sign, tz, ty)
        link, size = (axis, sign), (r1 - r0) * (c1 - c0) * 2
        self.task(("t",) + name, needs, 0.0, None, (name, link, size, at(rz, ry), at(tz, ty)))

    def cot(self, kind, piece, link, dx, half, needs):
        c = self.c
        h0, h1 = (0, 128) if half is None else ((0, 64), (64, 128))[half]

        def at():
            return c.cot.at[pl.ds(c.token_row(dx) + h0, h1 - h0), pl.ds(piece * 1024, 1024)]

        name = ("C", kind, piece, link)
        self.task(("t",) + name, needs, 0.0, None, (name, link, (h1 - h0) * 2048, at, at))

    def gradient(self, cls, part, half, axis, sign, rz, ry, needs, ins):
        c = self.c
        tz, ty = step(rz, ry, axis, sign)
        name = (cls, half, sign, tz, ty)
        r0, r1 = grows(part, half)
        self.rows[name] = (r0, r1, self.total_rows)
        self.total_rows += r1 - r0
        self.task(
            ("t",) + name,
            list(needs) + list(ins),
            0.05,
            lambda: c.add(part, r0, r1, block_at(rz, ry), ins, name),
            (name, (axis, sign), (r1 - r0) * 256, lambda: c.slot("send", name), lambda: c.slot("recv", name)),
        )

    def build(self):
        c, weight, cot, task, gradient = self.c, self.weight, self.cot, self.task, self.gradient
        task("start", [], 4.0, lambda: c.start())
        start = ["start"]
        arrived = []
        for s in BOTH:
            h = 0 if s == 1 else 1
            weight(0, 0, "B", None, "z", s, start)
            for hop in (1, 2, 3):
                weight(-s * hop, 0, "B", h if hop == 3 else None, "z", s, [("W", "B", "z", s, -s * hop, 0)])
            for rz in [0, -1, 1, -2, 2, -3, 3, 4]:
                if rz == 0:
                    needs = start
                elif rz == 4:
                    needs = [("W", "B", "z", t, 4, 0) for t in BOTH]
                else:
                    needs = [("W", "B", "z", 1 if rz < 0 else -1, rz, 0)]
                weight(rz, 0, "B", None, "y", s, needs)
                weight(rz, -s, "B", h, "y", s, [("W", "B", "y", s, rz, -s)])
                arrived.append(("W", "B", "y", s, rz, 2))
            weight(0, 0, "A", None, "y", s, start)
            weight(0, -s, "A", h, "y", s, [("W", "A", "y", s, 0, -s)])
            for ry in YORDER:
                if ry == 0:
                    needs = start
                elif ry == 2:
                    needs = [("W", "A", "y", t, 0, 2) for t in BOTH]
                else:
                    needs = [("W", "A", "y", -ry, 0, ry)]
                weight(0, ry, "A", None, "z", s, needs)
                for hop in (1, 2, 3):
                    weight(-s * hop, ry, "A", h if hop == 3 else None, "z", s, [("W", "A", "z", s, -s * hop, ry)])
                arrived.append(("W", "A", "z", s, 4, ry))
        for k in range(4):
            task(("load", k), start, 0.0, lambda k=k: c.wait_cot_load(k))
            for s in BOTH:
                h = 0 if s == 1 else 1
                own = ("C", "own", k, ("x", s))
                cot("own", k, ("x", s), 0, None, [("load", k)])
                cot("forward", k, ("x", s), -s, h, [own])
                cot("side%d" % s, k, ("c", 1), -s, None, [own])
                cot("far%d" % s, k, ("c", 1), -2 * s, h, [("C", "forward", k, ("x", s))])
            cot("own", k, ("c", 1), 0, None, [("load", k)])
        task("hidden", start, 2.0, lambda: c.hidden())
        for i, rz in enumerate(ZORDER):
            k = i // 2
            pieces = [("C", kind, k, ("c", 1)) for kind in ("own", "side1", "side-1", "far1", "far-1")]
            pieces += [("C", kind, k, ("x", s)) for kind in ("own", "forward") for s in BOTH]
            task(("down", rz), ["hidden", ("load", k)] + pieces, 1.0, lambda i=i: c.down_product(i))
        for i in range(4):
            task(("hg", i), arrived + [("down", rz) for rz in (4, -3, -2, 0)], 2.1, lambda i=i: c.hidden_grad(i))
        for ry in YORDER:
            for s in BOTH:
                h = 0 if s == 1 else 1
                gradient("A1", "A", h, "z", s, 4, ry, [("down", 4)], [])
                gradient("A1", "A", 1 - h, "z", s, 3 * s, ry, [("down", 3 * s)], [])
                gradient("A1", "A", h, "z", s, 3 * s, ry, [("down", 3 * s)], [("A1", h, s, 3 * s, ry)])
                gradient("A1", "A", None, "z", s, 2 * s, ry, [("down", 2 * s)], [("A1", v, s, 2 * s, ry) for v in (0, 1)])
                gradient("A1", "A", None, "z", s, s, ry, [("down", s)], [("A1", None, s, s, ry)])
            ins = [("A1", None, s, 0, ry) for s in BOTH]
            if ry == 2:
                for s in BOTH:
                    gradient("A2", "A", 0 if s == 1 else 1, "y", s, 0, 2, [("down", 0)], ins)
            elif ry:
                h = 0 if ry == 1 else 1
                gradient("A2", "A", 1 - h, "y", ry, 0, ry, [("down", 0)], ins)
                gradient("A2", "A", h, "y", ry, 0, ry, [("down", 0)], ins + [("A2", h, ry, 0, ry)])
            else:
                ins = ins + [("A2", v, s, 0, 0) for s in BOTH for v in (0, 1)]
                task("finalA", ins + [("down", 0)], 0.05, lambda ins=ins: c.add("A", *grows("A", None), block_at(0, 0), ins, None))
        for rz in ZORDER:
            for s in BOTH:
                h = 0 if s == 1 else 1
                gradient("B1", "B", h, "y", s, rz, 2, [("down", rz)], [])
                gradient("B1", "B", 1 - h, "y", s, rz, s, [("down", rz)], [])
                gradient("B1", "B", h, "y", s, rz, s, [("down", rz)], [("B1", h, s, rz, s)])
            ins = [("B1", v, s, rz, 0) for s in BOTH for v in (0, 1)]
            if rz == 4:
                for s in BOTH:
                    gradient("B2", "B", 0 if s == 1 else 1, "z", s, 4, 0, [("down", 4)], ins)
            elif rz:
                s = 1 if rz > 0 else -1
                h = 0 if s == 1 else 1
                if abs(rz) == 3:
                    gradient("B2", "B", 1 - h, "z", s, rz, 0, [("down", rz)], ins)
                    gradient("B2", "B", h, "z", s, rz, 0, [("down", rz)], ins + [("B2", h, s, rz, 0)])
                elif abs(rz) == 2:
                    gradient("B2", "B", None, "z", s, rz, 0, [("down", rz)], ins + [("B2", v, s, rz, 0) for v in (0, 1)])
                else:
                    gradient("B2", "B", None, "z", s, rz, 0, [("down", rz)], ins + [("B2", None, s, rz, 0)])
            else:
                ins = ins + [("B2", None, s, 0, 0) for s in BOTH]
                task("finalB", ins + [("down", 0)], 0.05, lambda ins=ins: c.add("B", *grows("B", None), block_at(0, 0), ins, None))


class Nothing:
    pass


class Kernel:
    def __init__(self, refs, scale):
        self.__dict__.update(refs)
        self.scale = scale
        self.z, self.y, self.x, self.core = (lax.axis_index(a) for a in ("z", "y", "x", "core"))

    def token_row(self, dx):
        return pl.multiple_of(lax.rem(self.x + dx + NX, NX) * 256 + self.core * 128, 128)

    def device(self, link):
        axis, sign = link
        if axis == "c":
            return {"core": 1 - self.core}
        size = {"z": NZ, "y": NY, "x": NX}[axis]
        return {axis: lax.rem(getattr(self, axis) + sign + size, size)}

    def local(self, src, dst, sem):
        copy = pltpu.make_async_copy(src, dst, self.lsem.at[sem])
        copy.start()
        return copy

    def start(self):
        barrier = pltpu.get_barrier_semaphore()
        for link in LINKS:
            pl.semaphore_signal(barrier, inc=1, device_id=self.device(link), device_id_type=pl.DeviceIdType.MESH)
        w_load = self.local(self.w_hbm, self.w.at[pl.ds(block_at(0, 0) * 128, 128)], 0)
        self.load_cot()
        pl.semaphore_wait(barrier, BARRIER)
        w_load.wait()

    def load_cot(self):
        own = self.token_row(0)
        for i, rz in enumerate(ZORDER):
            for j, ry in enumerate(YORDER):
                col = (lax.rem(self.z + rz + NZ, NZ) * NY + lax.rem(self.y + ry + NY, NY)) * 128
                b = i * 4 + j
                source = self.cot_hbm.at[:, pl.ds(pl.multiple_of(col, 128), 128)]
                self.local(source, self.cot.at[pl.ds(own, 128), pl.ds(b * 128, 128)], 3 + b // 8)
        self.g_load = self.local(self.gate_hbm, self.gate, 1)
        self.u_load = self.local(self.up_hbm, self.up, 2)

    def wait_cot_load(self, k):
        piece = self.cot.at[pl.ds(0, 128), pl.ds(k * 1024, 1024)]
        pltpu.make_async_copy(piece, piece, self.lsem.at[3 + k]).wait()

    def hidden(self):
        self.g_load.wait()
        self.u_load.wait()

        def body(i, carry):
            rows = pl.ds(pl.multiple_of(i * 128, 128), 128)
            for n in range(6):
                cols = pl.ds(n * 128, 128)
                g = self.gate[rows, cols].astype(F32)
                u = self.up[rows, cols].astype(F32)
                s = jax.nn.sigmoid(g)
                silu = g * s
                self.ht[cols, rows] = (silu * u).T.astype(BF16)
                self.to_up[rows, cols] = 0.5 * silu
                self.to_gate[rows, cols] = 0.5 * (u * s * (1.0 + g * (1.0 - s)))
            return carry

        lax.fori_loop(0, 8, body, 0)

    def down_product(self, z):
        for half in range(2):
            b = z * 4 + half * 2
            res = jnp.dot(self.ht[...], self.cot[:, pl.ds(b * 128, 256)], preferred_element_type=F32)
            self.part[b] = res[:, :128]
            self.part[b + 1] = res[:, 128:]

    def slot(self, side, name):
        r0, r1, offset = self.rows[name]
        return self.buffers[side].at[pl.ds(offset, r1 - r0)]

    def add(self, part, r0, r1, block, ins, name):
        spans = [self.rows[n] for n in ins]
        edges = {r0, r1} | {e for s0, s1, _ in spans for e in (s0, s1) if r0 < e < r1}
        cuts = sorted(edges)
        for a, b in zip(cuts, cuts[1:]):
            total = self.part[block, pl.ds(a, b - a)]
            for s0, s1, offset in spans:
                if a >= s0 and b <= s1:
                    total = total + decode(self.buffers["recv"][pl.ds(offset + a - s0, b - a)])
            if name is None:
                self.total[pl.ds(a, b - a)] = total
            else:
                s0, _, offset = self.rows[name]
                self.buffers["send"][pl.ds(offset + a - s0, b - a)] = encode(total)

    def hidden_grad(self, i):
        def multiply(j, carry):
            rows = pl.ds(pl.multiple_of(i * 256 + j * 128, 128), 128)
            for n in range(3):
                cols = pl.ds(n * 256, 256)
                here = pl.ds(pl.multiple_of(j * 128, 128), 128)
                self.acc[here, cols] = jnp.dot(self.cot[rows], self.w[:, cols], preferred_element_type=F32)
            return carry

        def finish(j, carry):
            rows = pl.ds(pl.multiple_of(i * 256 + j * 32, 32), 32)
            grad = self.acc[pl.ds(pl.multiple_of(j * 32, 32), 32)]
            self.up_out[rows] = (grad * self.to_up[rows]).astype(BF16)
            self.gate_out[rows] = (grad * self.to_gate[rows]).astype(BF16)
            return carry

        lax.fori_loop(0, 2, multiply, 0)
        lax.fori_loop(0, 8, finish, 0, unroll=2)

    def finish(self):
        for n in range(6):
            rows = pl.ds(n * 128, 128)
            self.down_out[:, rows] = self.total[rows].T * self.scale


def kernel(scale, cot_hbm, gate_hbm, up_hbm, w_hbm, gate_out, up_out, down_out, cot, w, part, gate, up, to_gate, to_up, ht, acc, total, sb, rb, ssem, rsem, lsem):
    refs = dict(
        cot_hbm=cot_hbm, gate_hbm=gate_hbm, up_hbm=up_hbm, w_hbm=w_hbm,
        cot=cot, w=w, part=part, gate=gate, up=up, to_gate=to_gate, to_up=to_up, ht=ht,
        gate_out=gate_out, up_out=up_out, acc=acc, total=total, down_out=down_out, lsem=lsem,
        buffers={"send": sb, "recv": rb},
    )
    c = Kernel(refs, scale)
    p = Tasks(c)
    c.rows = p.rows
    waited, sent, done = set(), set(), set()
    assert sorted(ORDER) == list(range(len(p.tasks)))

    def all_of(kind, elements):
        ref = {"W": w, "C": cot}.get(kind, rb)
        assert elements % ref.shape[1] == 0
        return ref.at[pl.ds(0, elements // ref.shape[1])]

    def remote(src, dst, send, receive, link):
        return pltpu.make_async_remote_copy(
            src_ref=src,
            dst_ref=dst,
            send_sem=ssem.at[send],
            recv_sem=rsem.at[receive],
            device_id=c.device(link),
            device_id_type=pl.DeviceIdType.MESH,
        )

    for t in ORDER:
        name, needs, _, function, message = p.tasks[t]
        for need in needs:
            if need in p.message:
                key = receive_group(need)
                if key not in waited:
                    assert all(m in sent for m in p.message if receive_group(m) == key)
                    ref = all_of(need[0], p.group_size[key])
                    remote(ref, ref, 0, p.groups[key], LINKS[0]).wait_recv()
                    waited.add(key)
            else:
                assert need in done, need
        if function:
            function()
        if message:
            m, link, _, src, dst = message
            remote(src(), dst(), send_group(m), p.groups[receive_group(m)], link).start()
            sent.add(m)
        done.add(name)
    assert waited == set(p.groups), set(p.groups) - waited
    c.finish()
    for i, kind in enumerate("WCG"):
        ref = all_of(kind, p.sent[i])
        remote(ref, ref, i, 0, LINKS[0]).wait_send()


def copy_out(gate_in, up_in, down_in, gate_grad, up_grad, down_grad, sem):
    pairs = [(gate_in, gate_grad), (up_in, up_grad), (down_in, down_grad)]
    copies = []
    for src, dst in pairs:
        height = src.shape[0] // 4
        for i in range(4):
            rows = pl.ds(i * height, height)
            copies.append(pltpu.make_async_copy(src.at[rows], dst.at[rows], sem.at[len(copies)]))
    for copy in copies:
        copy.start()
    for copy in copies:
        copy.wait()


def local(cotangent, gate_pre, up_pre, down_weight):
    tokens = gate_pre.shape[0] * NZ * NY
    p = Tasks(Nothing())
    hbm = pl.BlockSpec(memory_space=pl.ANY)

    def body(*refs):
        kernel(0.5 / math.sqrt(tokens), *refs)

    results = pl.pallas_call(
        body,
        out_shape=tuple(pltpu.VMEM(*o) for o in OUTPUTS),
        in_specs=[hbm] * 4,
        out_specs=[pl.BlockSpec(memory_space=pltpu.VMEM)] * 3,
        scratch_shapes=[
            pltpu.VMEM((1024, 4096), BF16),
            pltpu.VMEM((4096, 768), BF16),
            pltpu.VMEM((32, 768, 128), F32),
            pltpu.VMEM((1024, 768), BF16),
            pltpu.VMEM((1024, 768), BF16),
            pltpu.VMEM((1024, 768), F32),
            pltpu.VMEM((1024, 768), F32),
            pltpu.VMEM((768, 1024), BF16),
            pltpu.VMEM((256, 768), F32),
            pltpu.VMEM((768, 128), F32),
            pltpu.VMEM((p.total_rows, 128), BF16),
            pltpu.VMEM((p.total_rows, 128), BF16),
            pltpu.SemaphoreType.DMA((3,)),
            pltpu.SemaphoreType.DMA((len(p.groups),)),
            pltpu.SemaphoreType.DMA((7,)),
        ],
        compiler_params=pltpu.CompilerParams(
            collective_id=0, has_side_effects=True, vmem_limit_bytes=LIMIT
        ),
        name="gated_backward",
    )(cotangent, gate_pre, up_pre, down_weight)
    return pl.pallas_call(
        copy_out,
        out_shape=tuple(jax.ShapeDtypeStruct(*o) for o in OUTPUTS),
        in_specs=[pl.BlockSpec(memory_space=pltpu.VMEM)] * 3,
        out_specs=[hbm] * 3,
        scratch_shapes=[pltpu.SemaphoreType.DMA((12,))],
        compiler_params=pltpu.CompilerParams(vmem_limit_bytes=1 << 20),
        name="copy_out",
    )(*results)


def solution(mesh):
    torus = Mesh(mesh.devices.reshape(NZ, NY, NX, 2), ("z", "y", "x", "core"))
    rows, columns = ("z", "y"), ("x", "core")
    return jax.shard_map(
        local,
        mesh=torus,
        in_specs=(P(rows + columns, None), P(rows, columns), P(rows, columns), P(rows, columns)),
        out_specs=(P(rows, columns), P(rows, columns), P(rows, columns)),
        check_vma=False,
    )
```
